32 devices in a mesh: fs: 8 (over z, y), tp: 4 (over x, core).
Axes of the slice: x: 2, y: 2, z: 4, core: 2. Of those that a mesh axis runs over, the one named last changes fastest.
Arguments:
- inputs: bfloat16 [8192, 2304], P('fs'), may hold values from -6 to 6
- query_cot: bfloat16 [8192, 1024], P('fs', 'tp'), may hold values from -6 to 6
- head_out: bfloat16 [8192, 1024], P('fs', 'tp'), may hold values from -6 to 6
- out_cot: bfloat16 [8192, 2304], P('fs'), may hold values from -6 to 6
- query_factor: bfloat16 [2304, 192], P('fs'), may hold values from -2.5 to 2.5
- out_factor: bfloat16 [2304, 192], P('fs'), may hold values from -2.5 to 2.5
- query_master: float32 [2304, 1024], P('fs', 'tp'), may hold values from -0.125 to 0.125
- out_master: float32 [2304, 1024], P('fs', 'tp'), may hold values from -0.1875 to 0.1875
- query_first: float32 [192, 1024], P('fs', 'tp'), may hold values from -6 to 6
- query_second: float32 [192, 1024], P('fs', 'tp'), may hold values from 0.3 to 3
- out_first: float32 [192, 1024], P('fs', 'tp'), may hold values from -6 to 6
- out_second: float32 [192, 1024], P('fs', 'tp'), may hold values from 0.3 to 3
Outputs:
- query_step: float32 [2304, 1024], P('fs', 'tp')
- out_step: float32 [2304, 1024], P('fs', 'tp')
- query_copy: bfloat16 [2304, 1024], P(None, 'tp')
- out_copy: bfloat16 [2304, 1024], P(None, 'tp')
- query_first_new: float32 [192, 1024], P('fs', 'tp')
- query_second_new: float32 [192, 1024], P('fs', 'tp')
- out_first_new: float32 [192, 1024], P('fs', 'tp')
- out_second_new: float32 [192, 1024], P('fs', 'tp')
The draws below stay inside these ranges and needn't reach their ends.
All inputs are finite; a program needn't handle non-finite values.
Results may differ from the reference program's by a relative error of at most 0.0065.
Values may be sent and summed in bfloat16 or wider, within the bound.
A program may use at most 64 MiB of HBM per device.

```python
import math
import jax
import jax.numpy as jnp
from jax import lax

D = 2304
RANK = 192
QC = 1024
TOKENS = 8192


def factor_table(key):
    base = jax.random.truncated_normal(jax.random.fold_in(key, 11), -4.0, 4.0, (D, RANK), jnp.float32)
    base = base * D ** (-0.5)
    rising = 3.0 ** (jnp.arange(RANK, dtype=jnp.float32) / RANK)
    rough = jnp.exp(jax.random.uniform(jax.random.fold_in(key, 12), (RANK,), jnp.float32, 0.0, math.log(3.3)))
    table = base * (rising * rough)[None, :]
    return table.astype(jnp.bfloat16)


def draw_query_factor(key, part):
    return factor_table(jax.random.fold_in(key, 1))


def draw_out_factor(key, part):
    return factor_table(jax.random.fold_in(key, 2))


def with_spikes(values, own_key, source, target, parts, factor):
    def block_of(axis_at):
        return (jnp.arange(values.shape[axis_at]) // (values.shape[axis_at] // parts)).reshape((-1,) + (1,) * (values.ndim - 1 - axis_at))

    first = jax.random.permutation(own_key, parts)[block_of(target)]
    second = (block_of(target) + parts // 2) % parts
    return jnp.where((block_of(source) == first) | (block_of(source) == second), factor * values, values)


def steps_of(rng, extent, shards, smallest, largest):
    def one(dim, blocks):
        draws = jax.random.uniform(jax.random.fold_in(jax.random.fold_in(rng, 6), dim), (blocks,), jnp.float32, smallest / len(shards), largest / len(shards))
        return jnp.repeat(jnp.exp(draws), extent[dim] // blocks).reshape((-1,) + (1,) * (len(extent) - dim - 1))

    level = one(*shards[0])
    for cut in shards[1:]:
        level = level * one(*cut)
    return level


def normal_values(rng, dims, spread, reach, shards=(), kind=jnp.bfloat16):
    gain = steps_of(rng, dims, shards, -0.22, 0.18) if shards else 1.0
    result = jax.random.normal(rng, dims, jnp.float32) * spread * gain
    return jnp.minimum(jnp.maximum(result, -reach), reach).astype(kind)


def heavy_noise(rng, extent, scale, limit, shards, heavy, kind=jnp.bfloat16):
    values = scale * jax.random.normal(rng, extent, jnp.float32)
    if shards:
        values = values * steps_of(rng, extent, shards, -0.22, 0.18)
    return jnp.clip(with_spikes(values, jax.random.fold_in(rng, 3), *heavy), -limit, limit).astype(kind)


def setup_inputs(seed: int = 0) -> dict:
    key_list = jax.random.split(jax.random.key(seed), 13)
    inputs = heavy_noise(key_list[0], (TOKENS, D), 1.0, 6.0, ((0, 8),), (0, 1, 8, 2.0))
    query_cot = normal_values(key_list[1], (TOKENS, QC), 1.0, 6.0, ((0, 8), (1, 4)))
    head_out = normal_values(key_list[2], (TOKENS, QC), 1.0, 6.0, ((0, 8), (1, 4)))
    out_cot = normal_values(key_list[3], (TOKENS, D), 1.0, 6.0, ((0, 8),))
    query_factor = draw_query_factor(jax.random.fold_in(key_list[12], 71), 0)
    out_factor = draw_out_factor(jax.random.fold_in(key_list[12], 71), 0)
    query_master = normal_values(key_list[6], (D, QC), D ** -0.5, 0.125, ((0, 8), (1, 4)), jnp.float32)
    out_master = normal_values(key_list[7], (D, QC), QC ** -0.5, 0.1875, ((0, 8), (1, 4)), jnp.float32)
    query_first = normal_values(key_list[8], (RANK, QC), 1.0, 6.0, ((0, 8), (1, 4)), jnp.float32)
    query_second = jnp.clip(jnp.exp(math.log(3.0) - 2.3025851 * jax.random.uniform(key_list[9], (RANK, QC), jnp.float32) ** steps_of(key_list[9], (RANK, QC), ((0, 8), (1, 4)), -0.2, 0.2)), 0.3, 3.0)
    out_first = normal_values(key_list[10], (RANK, QC), 1.0, 6.0, ((0, 8), (1, 4)), jnp.float32)
    out_second = jnp.clip(jnp.exp(math.log(3.0) - 2.3025851 * jax.random.uniform(key_list[11], (RANK, QC), jnp.float32) ** steps_of(key_list[11], (RANK, QC), ((0, 8), (1, 4)), -0.2, 0.2)), 0.3, 3.0)
    return dict(inputs=inputs, query_cot=query_cot, head_out=head_out, out_cot=out_cot, query_factor=query_factor, out_factor=out_factor, query_master=query_master, out_master=out_master, query_first=query_first, query_second=query_second, out_first=out_first, out_second=out_second)


beta_first = 0.8
beta_second = 0.95
adam_eps = 1e-08
learn_rate = 0.05
norm_eps = 1e-06

def moment_update(normed, first_old, second_old):
    first_new = beta_first * first_old + (1.0 - beta_first) * normed
    second_new = beta_second * second_old + (1.0 - beta_second) * normed * normed
    direction = (first_new / (jnp.sqrt(second_new) + adam_eps)).astype(jnp.bfloat16)
    return (first_new, second_new, direction)

def reference(inputs, query_cot, head_out, out_cot, query_factor, out_factor, query_master, out_master, query_first, query_second, out_first, out_second):
    grad_query = jnp.dot(inputs.T, query_cot, preferred_element_type=jnp.float32)
    proj_query = jnp.dot(query_factor.astype(jnp.float32).T, grad_query, precision=lax.Precision.HIGHEST)
    cot_low = jnp.dot(out_cot, out_factor, preferred_element_type=jnp.float32).astype(jnp.bfloat16)
    proj_out = jnp.dot(cot_low.T, head_out, preferred_element_type=jnp.float32)
    squares = jnp.sum(proj_query * proj_query) + jnp.sum(proj_out * proj_out)
    rms_value = jnp.sqrt(squares / (2.0 * RANK * QC) + norm_eps)
    first_q, second_q, dir_query = moment_update(proj_query / rms_value, query_first, query_second)
    first_o, second_o, dir_out = moment_update(proj_out / rms_value, out_first, out_second)
    query_step = jnp.dot(query_factor, dir_query, preferred_element_type=jnp.float32)
    out_step = jnp.dot(out_factor, dir_out, preferred_element_type=jnp.float32)
    query_copy = (query_master - learn_rate * query_step).astype(jnp.bfloat16)
    out_copy = (out_master - learn_rate * out_step).astype(jnp.bfloat16)
    return (query_step, out_step, query_copy, out_copy, first_q, second_q, first_o, second_o)
```

```python
import functools
import math

import jax
import jax.numpy as jnp
from jax import lax
from jax.experimental import pallas as pl
from jax.experimental.pallas import tpu as pltpu
from jax.sharding import PartitionSpec as P

beta_first = 0.8
beta_second = 0.95
adam_eps = 1e-08
learn_rate = 0.05
norm_eps = 1e-06
contract_rows = (((0,), (0,)), ((), ()))
MESH = pl.DeviceIdType.MESH


def split_axis(n):
    ny = max(d for d in range(1, math.isqrt(n) + 1) if n % d == 0)
    return n // ny, ny


def kernel(
    n, tp, count,
    inputs, out_cot, query_factor, out_factor,
    query_cot, head_out, query_master, out_master,
    query_first, query_second, out_first, out_second,
    factors, masters, direction, first_q, second_q, first_o, second_o,
    xbuf, lows, terms, parts, got, squares, dirs, whole,
    local_sem, low_sem, fz_send, fz_recv, fy_send, fy_recv, fc_sem,
    mz_send, mz_recv, my_send, my_recv, rs_send, rs_recv, ss_sem, ag_send, ag_recv,
):
    nz, ny = split_axis(n)
    me, t = lax.axis_index("fs"), lax.axis_index("tp")
    z, y = me // ny, lax.rem(me, ny)
    core = lax.rem(t, 2)
    other = t + 1 - 2 * core
    total = n * tp
    mine = me * tp + t
    own = first_q.shape[0]

    @pl.when(core == 0)
    def _():
        pltpu.make_async_copy(query_factor, factors.at[core, me], local_sem.at[0]).start()
        pltpu.make_async_copy(inputs, xbuf, local_sem.at[1]).start()

    @pl.when(core == 1)
    def _():
        pltpu.make_async_copy(out_factor, factors.at[core, me], local_sem.at[0]).start()
        pltpu.make_async_copy(out_cot, xbuf, local_sem.at[1]).start()

    barrier = pltpu.get_barrier_semaphore()

    def greet(i, c):
        k = lax.rem(mine + i, total)
        pl.semaphore_signal(
            barrier, inc=1, device_id={"fs": k // tp, "tp": lax.rem(k, tp)}, device_id_type=MESH
        )
        return c

    lax.fori_loop(1, total, greet, 0)
    masters[me, 0] = query_master[...].astype(jnp.bfloat16)
    masters[me, 1] = out_master[...].astype(jnp.bfloat16)
    pl.semaphore_wait(barrier, total - 1)
    pltpu.make_async_copy(query_factor, factors.at[core, me], local_sem.at[0]).wait()

    def remote(src, dst, send, recv, f, tt=None):
        where = {"fs": f} if tt is None else {"fs": f, "tp": tt}
        return pltpu.make_async_remote_copy(
            src_ref=src, dst_ref=dst, send_sem=send, recv_sem=recv,
            device_id=where, device_id_type=MESH,
        )

    def along_z(buf, dz, send, recv):
        return remote(
            buf.at[me], buf.at[me], send.at[dz], recv.at[z], lax.rem(z + dz, nz) * ny + y
        )

    def from_z(buf, dz, send, recv):
        src = lax.rem(z + nz - dz, nz)
        piece = buf.at[src * ny + y]
        return remote(piece, piece, send.at[dz], recv.at[src], src * ny + y)

    def along_y(buf, zz, dy, send, recv):
        piece = buf.at[zz * ny + y]
        return remote(
            piece, piece, send.at[zz, dy], recv.at[zz, y], z * ny + lax.rem(y + dy, ny)
        )

    def from_y(buf, zz, dy, send, recv):
        src = lax.rem(y + ny - dy, ny)
        piece = buf.at[zz * ny + src]
        return remote(piece, piece, send.at[zz, dy], recv.at[zz, src], z * ny + src)

    def send_z(buf, send, recv):
        def go(dz, c):
            along_z(buf, dz, send, recv).start()
            return c
        lax.fori_loop(1, nz, go, 0)

    def send_y(buf, zz, send, recv):
        def go(dy, c):
            along_y(buf, zz, dy, send, recv).start()
            return c
        lax.fori_loop(1, ny, go, 0)

    def forward(buf, sz, rz, sy, ry):
        def go(dz, c):
            from_z(buf, dz, sz, rz).wait_recv()
            send_y(buf, lax.rem(z + nz - dz, nz), sy, ry)
            return c
        lax.fori_loop(1, nz, go, 0)

    def finish_recv_y(buf, sy, ry):
        def go(k, c):
            from_y(buf, k // (ny - 1), 1 + lax.rem(k, ny - 1), sy, ry).wait_recv()
            return c
        lax.fori_loop(0, nz * (ny - 1), go, 0)

    def finish_send(buf, sz, rz, sy, ry):
        def go_z(dz, c):
            along_z(buf, dz, sz, rz).wait_send()
            return c
        lax.fori_loop(1, nz, go_z, 0)

        def go_y(k, c):
            along_y(buf, k // (ny - 1), 1 + lax.rem(k, ny - 1), sy, ry).wait_send()
            return c
        lax.fori_loop(0, nz * (ny - 1), go_y, 0)

    fac = factors.at[core]
    f_sems = (fz_send, fz_recv, fy_send, fy_recv)
    send_z(fac, fz_send, fz_recv)
    send_y(fac, z, fy_send, fy_recv)
    forward(fac, *f_sems)
    pltpu.make_async_copy(inputs, xbuf, local_sem.at[1]).wait()
    finish_recv_y(fac, fy_send, fy_recv)
    share = remote(fac, fac, fc_sem.at[0], fc_sem.at[1], me, other)
    share.start()

    rank = factors.shape[-1]
    width = factors.shape[1] * factors.shape[2]
    if factors.shape[2] % 16 == 0:
        table = factors[core].reshape(width, rank)
    else:
        table = factors[core].astype(jnp.float32).reshape(width, rank).astype(jnp.bfloat16)
    tokens = xbuf.shape[0]
    tile = math.gcd(tokens, 256)

    def fold(i, c):
        at = pl.ds(pl.multiple_of(i * tile, tile), tile)
        lows[core, at, :] = jnp.dot(
            xbuf[at, :], table, preferred_element_type=jnp.float32
        ).astype(jnp.bfloat16)
        return c

    lax.fori_loop(0, tokens // tile, fold, 0)
    swap = remote(lows.at[core], lows.at[core], low_sem.at[0], low_sem.at[1], me, other)
    swap.start()
    swap.wait_recv()

    terms[0] = lax.dot_general(lows[0], query_cot[...], contract_rows, preferred_element_type=jnp.float32)
    terms[1] = lax.dot_general(lows[1], head_out[...], contract_rows, preferred_element_type=jnp.float32)
    for j in range(n):
        for w in range(2):
            parts[j, w] = terms[w, j * own:(j + 1) * own, :].astype(jnp.bfloat16)

    def scatter(i):
        f = lax.rem(me + i, n)
        return remote(parts.at[f], got.at[me], rs_send.at[f], rs_recv.at[me], f)

    def scattered(i):
        f = lax.rem(me + i, n)
        return remote(parts.at[f], got.at[f], rs_send.at[f], rs_recv.at[f], f)

    def each(make, act):
        def go(i, c):
            act(make(i))
            return c
        lax.fori_loop(1, n, go, 0)

    each(scatter, lambda d: d.start())
    m_sems = (mz_send, mz_recv, my_send, my_recv)
    send_z(masters, mz_send, mz_recv)
    send_y(masters, z, my_send, my_recv)
    each(scattered, lambda d: d.wait_recv())

    got[me] = parts[me]

    def add(j, c):
        return c + got[j].astype(jnp.float32)

    proj = lax.fori_loop(0, n, add, jnp.zeros(got.shape[1:], jnp.float32))
    sq = proj * proj
    row = jnp.sum(jnp.sum(sq, axis=0), axis=0, keepdims=True)
    squares[mine] = sum(row[:, k:k + 128] for k in range(0, row.shape[1], 128))

    def tell(i, c):
        k = lax.rem(mine + i, total)
        remote(
            squares.at[mine], squares.at[mine], ss_sem.at[0], ss_sem.at[1],
            k // tp, lax.rem(k, tp),
        ).start()
        return c

    lax.fori_loop(1, total, tell, 0)
    rest = squares.at[pl.ds(0, total - 1)]
    pltpu.make_async_copy(rest, rest, ss_sem.at[1]).wait()
    rms = jnp.sqrt(jnp.sum(squares[...]) / count + norm_eps)

    olds = ((query_first, query_second), (out_first, out_second))
    news = ((first_q, second_q), (first_o, second_o))
    for w in range(2):
        normed = proj[w] / rms
        first = beta_first * olds[w][0][...] + (1.0 - beta_first) * normed
        second = beta_second * olds[w][1][...] + (1.0 - beta_second) * normed * normed
        news[w][0][...] = first
        news[w][1][...] = second
        dirs[me, w] = (first / (jnp.sqrt(second) + adam_eps)).astype(jnp.bfloat16)

    def spread(i):
        f = lax.rem(me + i, n)
        return remote(dirs.at[me], dirs.at[me], ag_send.at[f], ag_recv.at[me], f)

    def arrived(i):
        f = lax.rem(me + i, n)
        return remote(dirs.at[f], dirs.at[f], ag_send.at[f], ag_recv.at[f], f)

    each(spread, lambda d: d.start())
    forward(masters, *m_sems)
    each(arrived, lambda d: d.wait_recv())
    for w in range(2):
        for j in range(n):
            whole[j * own:(j + 1) * own, :] = dirs[j, w].astype(jnp.float32)
        direction[w] = whole[...].astype(jnp.bfloat16)

    finish_recv_y(masters, my_send, my_recv)
    back = factors.at[1 - core]
    remote(back, back, fc_sem.at[0], fc_sem.at[1], me, other).wait_recv()
    share.wait_send()
    swap.wait_send()
    finish_send(fac, *f_sems)
    finish_send(masters, *m_sems)
    each(scatter, lambda d: d.wait_send())
    each(spread, lambda d: d.wait_send())
    pltpu.make_async_copy(rest, rest, ss_sem.at[0]).wait()


def exchange(n, tp, inputs, out_cot, query_factor, out_factor, query_cot, head_out,
             query_master, out_master, *moments):
    rows, rank = query_factor.shape
    cols = query_cot.shape[1]
    own = moments[0].shape[0]
    tokens, width = inputs.shape
    nz, ny = split_axis(n)
    vmem = pl.BlockSpec(memory_space=pltpu.VMEM)
    anyspace = pl.BlockSpec(memory_space=pl.ANY)
    dma = pltpu.SemaphoreType.DMA
    bf, f32 = jnp.bfloat16, jnp.float32
    shape = jax.ShapeDtypeStruct
    return pl.pallas_call(
        functools.partial(kernel, n, tp, 2.0 * rank * cols * tp),
        out_shape=(
            shape((2, n, rows, rank), bf),
            shape((n, 2, rows, cols), bf),
            shape((2, rank, cols), bf),
            *(shape((own, cols), f32) for _ in range(4)),
        ),
        in_specs=[anyspace] * 4 + [vmem] * 8,
        out_specs=(vmem,) * 7,
        scratch_shapes=[
            pltpu.VMEM((tokens, width), bf),
            pltpu.VMEM((2, tokens, rank), bf),
            pltpu.VMEM((2, rank, cols), f32),
            pltpu.VMEM((n, 2, own, cols), bf),
            pltpu.VMEM((n, 2, own, cols), bf),
            pltpu.VMEM((n * tp, 1, 128), f32),
            pltpu.VMEM((n, 2, own, cols), bf),
            pltpu.VMEM((rank, cols), f32),
            dma((2,)), dma((2,)),
            dma((nz,)), dma((nz,)), dma((nz, ny)), dma((nz, ny)), dma((2,)),
            dma((nz,)), dma((nz,)), dma((nz, ny)), dma((nz, ny)),
            dma((n,)), dma((n,)), dma((2,)), dma((n,)), dma((n,)),
        ],
        compiler_params=pltpu.CompilerParams(
            collective_id=0, has_side_effects=True, vmem_limit_bytes=56 * 1024 * 1024
        ),
    )(inputs, out_cot, query_factor, out_factor, query_cot, head_out,
      query_master, out_master, *moments)


def body(
    n, tp, inputs, query_cot, head_out, out_cot, query_factor, out_factor,
    query_master, out_master, query_first, query_second, out_first, out_second,
):
    factors, masters, direction, first_q, second_q, first_o, second_o = exchange(
        n, tp, inputs, out_cot, query_factor, out_factor, query_cot, head_out,
        query_master, out_master, query_first, query_second, out_first, out_second,
    )
    rank = query_factor.shape[1]
    cols = query_cot.shape[1]

    def dot(a, b):
        return jnp.dot(a, b, preferred_element_type=jnp.float32)

    query_step = dot(query_factor, direction[0])
    out_step = dot(out_factor, direction[1])
    copies = []
    for w in range(2):
        step = dot(factors[w].reshape(-1, rank), direction[w])
        master = masters[:, w].reshape(-1, cols).astype(jnp.float32)
        copies.append((master - learn_rate * step).astype(jnp.bfloat16))
    return (query_step, out_step, *copies, first_q, second_q, first_o, second_o)


def solution(mesh):
    rows, both = P("fs", None), P("fs", "tp")
    return jax.shard_map(
        functools.partial(body, mesh.shape["fs"], mesh.shape["tp"]),
        mesh=mesh,
        in_specs=(rows, both, both, rows, rows, rows) + (both,) * 6,
        out_specs=(both, both, P(None, "tp"), P(None, "tp")) + (both,) * 4,
        check_vma=False,
    )
```

```python
import functools
import math

import jax
import jax.numpy as jnp
from jax import lax
from jax.experimental import pallas as pl
from jax.experimental.pallas import tpu as pltpu
from jax.sharding import PartitionSpec as P

beta_first = 0.8
beta_second = 0.95
adam_eps = 1e-08
learn_rate = 0.05
norm_eps = 1e-06
contract_rows = (((0,), (0,)), ((), ()))
MESH = pl.DeviceIdType.MESH


def shares_of(tp, rows):
    return tp // 2 if rows % (tp // 2 * 16) == 0 else 1


def split_axis(n):
    ny = max(d for d in range(1, math.isqrt(n) + 1) if n % d == 0)
    return n // ny, ny


def moments(normed, first, second):
    first_new = beta_first * first + (1.0 - beta_first) * normed
    second_new = beta_second * second + (1.0 - beta_second) * normed * normed
    return first_new, second_new


def finish(
    factors, masters, direction, normed, query_first, query_second, out_first, out_second,
    query_step, out_step, query_copy, out_copy, first_q, second_q, first_o, second_o,
):
    j = pl.program_id(0)

    @pl.when(j == 0)
    def _():
        first_q[...], second_q[...] = moments(normed[0], query_first[...], query_second[...])
        first_o[...], second_o[...] = moments(normed[1], out_first[...], out_second[...])

    for w, (step_out, copy) in enumerate(((query_step, query_copy), (out_step, out_copy))):
        step = jnp.dot(factors[w, 0], direction[w], preferred_element_type=jnp.float32)
        copy[...] = (masters[0, w].astype(jnp.float32) - learn_rate * step).astype(copy.dtype)

        @pl.when(j == lax.axis_index("fs"))
        def _():
            step_out[...] = step


def kernel(
    n, tp, count,
    inputs, out_cot, query_factor, out_factor,
    query_cot, head_out, query_master, out_master,
    query_first, query_second, out_first, out_second,
    factors, masters, direction, normed_out,
    xbuf, lows, terms, parts, got, squares, dirs, whole,
    local_sem, low_sem, fu_send, fd_send, fz_recv, fy_send, fy_recv, fx_send, fx_recv, fc_sem,
    mu_send, md_send, mz_recv, my_send, my_recv, rs_send, rs_recv, ss_sem, ag_send, ag_recv,
):
    nz, ny = split_axis(n)
    me, t = lax.axis_index("fs"), lax.axis_index("tp")
    z, y = me // ny, lax.rem(me, ny)
    core = lax.rem(t, 2)
    other = t + 1 - 2 * core
    total = n * tp
    mine = me * tp + t
    own = query_first.shape[0]

    def own_factor(source):
        return pltpu.make_async_copy(source, factors.at[core, me], local_sem.at[0])

    @pl.when(core == 0)
    def _():
        own_factor(query_factor).start()
        pltpu.make_async_copy(inputs, xbuf, local_sem.at[1]).start()

    @pl.when(core == 1)
    def _():
        own_factor(out_factor).start()
        pltpu.make_async_copy(out_cot, xbuf, local_sem.at[1]).start()

    barrier = pltpu.get_barrier_semaphore()

    def greet(i, c):
        k = lax.rem(mine + i, total)
        pl.semaphore_signal(
            barrier, inc=1, device_id={"fs": k // tp, "tp": lax.rem(k, tp)}, device_id_type=MESH
        )
        return c

    lax.fori_loop(1, total, greet, 0)
    masters[me, 0] = query_master[...].astype(jnp.bfloat16)
    masters[me, 1] = out_master[...].astype(jnp.bfloat16)
    pl.semaphore_wait(barrier, total - 1)
    own_factor(query_factor).wait()

    def remote(src, dst, send, recv, f, tt=None):
        where = {"fs": f} if tt is None else {"fs": f, "tp": tt}
        return pltpu.make_async_remote_copy(
            src_ref=src, dst_ref=dst, send_sem=send, recv_sem=recv,
            device_id=where, device_id_type=MESH,
        )

    def up(piece, zz, sems):
        return remote(piece(zz, y), piece(zz, y), sems[0].at[zz], sems[2].at[zz], me + ny)

    def down(piece, zz, sems):
        return remote(piece(zz, y), piece(zz, y), sems[1].at[zz], sems[2].at[zz], me - ny)

    def along_y(piece, zz, dy, sems):
        return remote(
            piece(zz, y), piece(zz, y), sems[3].at[zz, dy], sems[4].at[zz, y],
            z * ny + lax.rem(y + dy, ny),
        )

    def from_y(piece, zz, dy, sems):
        src = lax.rem(y + ny - dy, ny)
        return remote(
            piece(zz, src), piece(zz, src), sems[3].at[zz, dy], sems[4].at[zz, src], z * ny + src
        )

    def loop(low, high, act):
        def go(i, c):
            act(i)
            return c
        lax.fori_loop(low, high, go, 0)

    def hops(piece, low, high, sems, extra=None):
        def pass_on(zz, come, up_too, down_too):
            @pl.when(come)
            def _():
                @pl.when(zz != z)
                def _():
                    up(piece, zz, sems).wait_recv()

                @pl.when(up_too)
                def _():
                    up(piece, zz, sems).start()

                @pl.when(down_too)
                def _():
                    down(piece, zz, sems).start()

                loop(1, ny, lambda dy: along_y(piece, zz, dy, sems).start())
                if extra is not None:
                    extra(zz, y)

        def step(k):
            pass_on(z - k, z >= k, z < nz - 1, (k == 0) & (z > 0))
            pass_on(z + k, (k > 0) & (z + k < nz), z < 0, z > 0)

        loop(low, high, step)

    def all_y(act):
        loop(0, nz * (ny - 1), lambda k: act(k // (ny - 1), 1 + lax.rem(k, ny - 1)))

    def sent(piece, sems):
        @pl.when(z < nz - 1)
        def _():
            loop(0, z + 1, lambda zz: up(piece, zz, sems).wait_send())

        @pl.when(z > 0)
        def _():
            loop(z, nz, lambda zz: down(piece, zz, sems).wait_send())

        all_y(lambda zz, dy: along_y(piece, zz, dy, sems).wait_send())

    shares = factors.shape[2]
    part = lax.rem(t // 2, shares)

    def f_piece(zz, yy):
        return factors.at[core, zz * ny + yy, part]

    def m_piece(zz, yy):
        return masters.at[zz * ny + yy]

    def over_x(zz, yy, dx):
        block = zz * ny + yy
        piece = factors.at[core, block, part]
        return remote(
            piece, piece, fx_send.at[block, dx], fx_recv.at[block, part],
            me, 2 * lax.rem(part + dx, shares) + core,
        )

    def from_x(zz, yy, dx):
        block = zz * ny + yy
        src = lax.rem(part + shares - dx, shares)
        piece = factors.at[core, block, src]
        return remote(
            piece, piece, fx_send.at[block, dx], fx_recv.at[block, src], me, 2 * src + core
        )

    def send_x(zz, yy):
        @pl.when(zz * ny + yy != me)
        def _():
            for dx in range(1, shares):
                over_x(zz, yy, dx).start()

    f_sems = (fu_send, fd_send, fz_recv, fy_send, fy_recv)
    m_sems = (mu_send, md_send, mz_recv, my_send, my_recv)
    hops(f_piece, 0, nz, f_sems, send_x)
    hops(m_piece, 0, 1, m_sems)
    pltpu.make_async_copy(inputs, xbuf, local_sem.at[1]).wait()

    def take_y(zz, dy):
        from_y(f_piece, zz, dy, f_sems).wait_recv()
        send_x(zz, lax.rem(y + ny - dy, ny))

    all_y(take_y)

    def others(act):
        for dx in range(1, shares):
            loop(1, n, lambda i: act(lax.rem(me + i, n) // ny, lax.rem(me + i, ny), dx))

    others(lambda zz, yy, dx: from_x(zz, yy, dx).wait_recv())
    fac = factors.at[core]
    share = remote(fac, fac, fc_sem.at[0], fc_sem.at[1], me, other)
    share.start()

    rank = factors.shape[-1]
    width = inputs.shape[1]
    if factors.shape[3] % 16 == 0:
        table = factors[core].reshape(width, rank)
    else:
        table = factors[core].astype(jnp.float32).reshape(width, rank).astype(jnp.bfloat16)
    tokens = xbuf.shape[0]
    tile = math.gcd(tokens, 256)

    def fold(i, c):
        at = pl.ds(pl.multiple_of(i * tile, tile), tile)
        lows[core, at, :] = jnp.dot(
            xbuf[at, :], table, preferred_element_type=jnp.float32
        ).astype(jnp.bfloat16)
        return c

    lax.fori_loop(0, tokens // tile, fold, 0)
    swap = remote(lows.at[core], lows.at[core], low_sem.at[0], low_sem.at[1], me, other)
    swap.start()
    swap.wait_recv()

    terms[0] = lax.dot_general(lows[0], query_cot[...], contract_rows, preferred_element_type=jnp.float32)
    terms[1] = lax.dot_general(lows[1], head_out[...], contract_rows, preferred_element_type=jnp.float32)
    for j in range(n):
        for w in range(2):
            parts[j, w] = terms[w, j * own:(j + 1) * own, :].astype(jnp.bfloat16)

    def scatter(i):
        f = lax.rem(me + i, n)
        return remote(parts.at[f], got.at[me], rs_send.at[f], rs_recv.at[me], f)

    def scattered(i):
        f = lax.rem(me + i, n)
        return remote(parts.at[f], got.at[f], rs_send.at[f], rs_recv.at[f], f)

    def each(make, act):
        def go(i, c):
            act(make(i))
            return c
        lax.fori_loop(1, n, go, 0)

    each(scatter, lambda d: d.start())
    hops(m_piece, 1, 2, m_sems)
    each(scattered, lambda d: d.wait_recv())

    got[me] = parts[me]

    def add(j, c):
        return c + got[j].astype(jnp.float32)

    proj = lax.fori_loop(0, n, add, jnp.zeros(got.shape[1:], jnp.float32))
    sq = proj * proj
    row = jnp.sum(jnp.sum(sq, axis=0), axis=0, keepdims=True)
    squares[mine] = sum(row[:, k:k + 128] for k in range(0, row.shape[1], 128))

    def tell(i, c):
        k = lax.rem(mine + i, total)
        remote(
            squares.at[mine], squares.at[mine], ss_sem.at[0], ss_sem.at[1],
            k // tp, lax.rem(k, tp),
        ).start()
        return c

    lax.fori_loop(1, total, tell, 0)
    rest = squares.at[pl.ds(0, total - 1)]
    pltpu.make_async_copy(rest, rest, ss_sem.at[1]).wait()
    rms = jnp.sqrt(jnp.sum(squares[...]) / count + norm_eps)

    olds = ((query_first, query_second), (out_first, out_second))
    for w in range(2):
        normed = proj[w] / rms
        normed_out[w] = normed
        first, second = moments(normed, olds[w][0][...], olds[w][1][...])
        dirs[me, w] = (first / (jnp.sqrt(second) + adam_eps)).astype(jnp.bfloat16)

    def spread(i):
        f = lax.rem(me + i, n)
        return remote(dirs.at[me], dirs.at[me], ag_send.at[f], ag_recv.at[me], f)

    def arrived(i):
        f = lax.rem(me + i, n)
        return remote(dirs.at[f], dirs.at[f], ag_send.at[f], ag_recv.at[f], f)

    each(spread, lambda d: d.start())
    hops(m_piece, 2, nz, m_sems)
    each(arrived, lambda d: d.wait_recv())
    for w in range(2):
        for j in range(n):
            whole[j * own:(j + 1) * own, :] = dirs[j, w].astype(jnp.float32)
        direction[w] = whole[...].astype(jnp.bfloat16)

    all_y(lambda zz, dy: from_y(m_piece, zz, dy, m_sems).wait_recv())
    back = factors.at[1 - core]
    remote(back, back, fc_sem.at[0], fc_sem.at[1], me, other).wait_recv()
    share.wait_send()
    swap.wait_send()
    sent(f_piece, f_sems)
    sent(m_piece, m_sems)
    others(lambda zz, yy, dx: over_x(zz, yy, dx).wait_send())
    each(scatter, lambda d: d.wait_send())
    each(spread, lambda d: d.wait_send())
    pltpu.make_async_copy(rest, rest, ss_sem.at[0]).wait()


def exchange(n, tp, inputs, out_cot, query_factor, out_factor, query_cot, head_out,
             query_master, out_master, *olds):
    rows = query_master.shape[0]
    rank = query_factor.shape[-1]
    cols = query_cot.shape[1]
    own = olds[0].shape[0]
    tokens, width = inputs.shape
    nz, ny = split_axis(n)
    vmem = pl.BlockSpec(memory_space=pltpu.VMEM)
    anyspace = pl.BlockSpec(memory_space=pl.ANY)
    dma = pltpu.SemaphoreType.DMA
    bf, f32 = jnp.bfloat16, jnp.float32
    shares = shares_of(tp, rows)
    gather = (dma((nz,)), dma((nz,)), dma((nz,)), dma((nz, ny)), dma((nz, ny)))
    shape = jax.ShapeDtypeStruct
    return pl.pallas_call(
        functools.partial(kernel, n, tp, 2.0 * rank * cols * tp),
        out_shape=(
            shape((2, n, shares, rows // shares, rank), bf),
            shape((n, 2, rows, cols), bf),
            shape((2, rank, cols), bf),
            shape((2, own, cols), f32),
        ),
        in_specs=[anyspace] * 4 + [vmem] * 8,
        out_specs=(vmem,) * 4,
        scratch_shapes=[
            pltpu.VMEM((tokens, width), bf),
            pltpu.VMEM((2, tokens, rank), bf),
            pltpu.VMEM((2, rank, cols), f32),
            pltpu.VMEM((n, 2, own, cols), bf),
            pltpu.VMEM((n, 2, own, cols), bf),
            pltpu.VMEM((n * tp, 1, 128), f32),
            pltpu.VMEM((n, 2, own, cols), bf),
            pltpu.VMEM((rank, cols), f32),
            dma((2,)), dma((2,)),
            *gather, dma((n, shares)), dma((n, shares)), dma((2,)),
            *gather,
            dma((n,)), dma((n,)), dma((2,)), dma((n,)), dma((n,)),
        ],
        compiler_params=pltpu.CompilerParams(
            collective_id=0, has_side_effects=True, vmem_limit_bytes=56 * 1024 * 1024
        ),
    )(inputs, out_cot, query_factor, out_factor, query_cot, head_out,
      query_master, out_master, *olds)


def body(
    n, tp, inputs, query_cot, head_out, out_cot, query_factor, out_factor,
    query_master, out_master, query_first, query_second, out_first, out_second,
):
    rows = query_factor.shape[0]
    shares = shares_of(tp, rows)

    def split(factor):
        return factor.reshape(shares, rows // shares, -1)

    factors, masters, direction, normed = exchange(
        n, tp, inputs, out_cot, split(query_factor), split(out_factor), query_cot, head_out,
        query_master, out_master, query_first, query_second, out_first, out_second,
    )
    rank = query_factor.shape[1]
    own, cols = query_first.shape
    f32, bf = jnp.float32, jnp.bfloat16
    factors = factors.reshape(2, n, rows, rank)
    shape = jax.ShapeDtypeStruct

    def fixed(*dims):
        return pl.BlockSpec(dims, lambda j: (0,) * len(dims))

    block = pl.BlockSpec((rows, cols), lambda j: (j, 0))
    return pl.pallas_call(
        finish,
        grid=(n,),
        in_specs=[
            pl.BlockSpec((2, 1, rows, rank), lambda j: (0, j, 0, 0)),
            pl.BlockSpec((1, 2, rows, cols), lambda j: (j, 0, 0, 0)),
            fixed(2, rank, cols),
            fixed(2, own, cols),
        ] + [fixed(own, cols)] * 4,
        out_specs=[fixed(rows, cols)] * 2 + [block] * 2 + [fixed(own, cols)] * 4,
        out_shape=[shape((rows, cols), f32)] * 2
        + [shape((n * rows, cols), bf)] * 2
        + [shape((own, cols), f32)] * 4,
    )(factors, masters, direction, normed, query_first, query_second, out_first, out_second)


def solution(mesh):
    rows, both = P("fs", None), P("fs", "tp")
    return jax.shard_map(
        functools.partial(body, mesh.shape["fs"], mesh.shape["tp"]),
        mesh=mesh,
        in_specs=(rows, both, both, rows, rows, rows) + (both,) * 6,
        out_specs=(both, both, P(None, "tp"), P(None, "tp")) + (both,) * 4,
        check_vma=False,
    )
```

```python
import functools
import math

import jax
import jax.numpy as jnp
from jax import lax
from jax.experimental import pallas as pl
from jax.experimental.pallas import tpu as pltpu
from jax.sharding import PartitionSpec as P

beta_first = 0.8
beta_second = 0.95
adam_eps = 1e-08
learn_rate = 0.05
norm_eps = 1e-06
contract_rows = (((0,), (0,)), ((), ()))
MESH = pl.DeviceIdType.MESH


def shares_of(tp, rows):
    return tp // 2 if rows % (tp // 2 * 16) == 0 else 1


def split_axis(n):
    ny = max(d for d in range(1, math.isqrt(n) + 1) if n % d == 0)
    return n // ny, ny


def moments(normed, first, second):
    first_new = beta_first * first + (1.0 - beta_first) * normed
    second_new = beta_second * second + (1.0 - beta_second) * normed * normed
    return first_new, second_new


def finish(
    factors, masters, direction, normed, query_first, query_second, out_first, out_second,
    query_step, out_step, query_copy, out_copy, first_q, second_q, first_o, second_o,
):
    j = pl.program_id(0)

    @pl.when(j == 0)
    def _():
        first_q[...], second_q[...] = moments(normed[0], query_first[...], query_second[...])
        first_o[...], second_o[...] = moments(normed[1], out_first[...], out_second[...])

    me = lax.axis_index("fs")
    blocks, rows = factors.shape[1:3]

    def one(i, c):
        at = pl.ds(pl.multiple_of(i * rows, 8), rows)
        for w, (step_out, copy) in enumerate(((query_step, query_copy), (out_step, out_copy))):
            step = jnp.dot(factors[w, i], direction[w], preferred_element_type=jnp.float32)
            copy[at, :] = (masters[w, i].astype(jnp.float32) - learn_rate * step).astype(copy.dtype)

            @pl.when(j * blocks + i == me)
            def _():
                step_out[...] = step
        return c

    lax.fori_loop(0, blocks, one, 0)


def kernel(
    n, tp, count,
    inputs, out_cot, query_factor, out_factor,
    query_cot, head_out, query_master, out_master,
    query_first, query_second, out_first, out_second,
    factors, masters, direction, normed_out,
    xbuf, lows, terms, parts, got, squares, dirs, whole,
    local_sem, low_sem, fz_send, fz_recv, fy_send, fy_recv, fx_send, fx_recv, fc_sem,
    mu_send, md_send, mz_recv, my_send, my_recv, rs_send, rs_recv, ss_sem, ag_send, ag_recv,
):
    nz, ny = split_axis(n)
    me, t = lax.axis_index("fs"), lax.axis_index("tp")
    z, y = me // ny, lax.rem(me, ny)
    core = lax.rem(t, 2)
    other = t + 1 - 2 * core
    total = n * tp
    mine = me * tp + t
    own = query_first.shape[0]

    def own_factor(source):
        return pltpu.make_async_copy(source, factors.at[core, me], local_sem.at[0])

    @pl.when(core == 0)
    def _():
        own_factor(query_factor).start()
        pltpu.make_async_copy(inputs, xbuf, local_sem.at[1]).start()

    @pl.when(core == 1)
    def _():
        own_factor(out_factor).start()
        pltpu.make_async_copy(out_cot, xbuf, local_sem.at[1]).start()

    barrier = pltpu.get_barrier_semaphore()

    def greet(f, tt):
        pl.semaphore_signal(
            barrier, inc=1, device_id={"fs": f, "tp": tt}, device_id_type=MESH
        )

    def loop(low, high, act):
        def go(i, c):
            act(i)
            return c
        lax.fori_loop(low, high, go, 0)

    shares = factors.shape[2]
    if shares == tp // 2:
        loop(1, nz, lambda i: greet(lax.rem(z + i, nz) * ny + y, t))
        loop(1, ny, lambda i: greet(z * ny + lax.rem(y + i, ny), t))
        loop(1, shares, lambda i: greet(me, lax.rem(t + 2 * i, tp)))
        greet(me, other)
        greeted = nz + ny + shares - 2
    else:
        loop(1, total, lambda i: greet(lax.rem(mine + i, total) // tp, lax.rem(mine + i, tp)))
        greeted = total - 1
    masters[0, me] = query_master[...].astype(jnp.bfloat16)
    masters[1, me] = out_master[...].astype(jnp.bfloat16)
    pl.semaphore_wait(barrier, greeted)
    own_factor(query_factor).wait()

    def remote(src, dst, send, recv, f, tt=None):
        where = {"fs": f} if tt is None else {"fs": f, "tp": tt}
        return pltpu.make_async_remote_copy(
            src_ref=src, dst_ref=dst, send_sem=send, recv_sem=recv,
            device_id=where, device_id_type=MESH,
        )

    def up(piece, zz, sems):
        return remote(piece(zz, y), piece(zz, y), sems[0].at[zz], sems[2].at[zz], me + ny)

    def down(piece, zz, sems):
        return remote(piece(zz, y), piece(zz, y), sems[1].at[zz], sems[2].at[zz], me - ny)

    def along_y(piece, zz, dy, sems):
        return remote(
            piece(zz, y), piece(zz, y), sems[3].at[zz, dy], sems[4].at[zz, y],
            z * ny + lax.rem(y + dy, ny),
        )

    def from_y(piece, zz, dy, sems):
        src = lax.rem(y + ny - dy, ny)
        return remote(
            piece(zz, src), piece(zz, src), sems[3].at[zz, dy], sems[4].at[zz, src], z * ny + src
        )

    def hops(piece, low, high, sems):
        def pass_on(zz, come, up_too, down_too):
            @pl.when(come)
            def _():
                @pl.when(zz != z)
                def _():
                    up(piece, zz, sems).wait_recv()

                @pl.when(up_too)
                def _():
                    up(piece, zz, sems).start()

                @pl.when(down_too)
                def _():
                    down(piece, zz, sems).start()

                loop(1, ny, lambda dy: along_y(piece, zz, dy, sems).start())

        def step(k):
            pass_on(z - k, z >= k, z < nz - 1, (k == 0) & (z > 0))
            pass_on(z + k, (k > 0) & (z + k < nz), z < 0, z > 0)

        loop(low, high, step)

    def all_y(act):
        loop(0, nz * (ny - 1), lambda k: act(k // (ny - 1), 1 + lax.rem(k, ny - 1)))

    def sent(piece, sems):
        @pl.when(z < nz - 1)
        def _():
            loop(0, z + 1, lambda zz: up(piece, zz, sems).wait_send())

        @pl.when(z > 0)
        def _():
            loop(z, nz, lambda zz: down(piece, zz, sems).wait_send())

        all_y(lambda zz, dy: along_y(piece, zz, dy, sems).wait_send())

    part = lax.rem(t // 2, shares)

    def f_piece(zz, yy):
        return factors.at[core, zz * ny + yy, part]

    def q_piece(zz, yy):
        return masters.at[0, zz * ny + yy]

    def o_piece(zz, yy):
        return masters.at[1, zz * ny + yy]

    def over_x(zz, yy, dx):
        block = zz * ny + yy
        piece = factors.at[core, block, part]
        return remote(
            piece, piece, fx_send.at[block, dx], fx_recv.at[block, part],
            me, 2 * lax.rem(part + dx, shares) + core,
        )

    def from_x(zz, yy, dx):
        block = zz * ny + yy
        src = lax.rem(part + shares - dx, shares)
        piece = factors.at[core, block, src]
        return remote(
            piece, piece, fx_send.at[block, dx], fx_recv.at[block, src], me, 2 * src + core
        )

    def send_x(zz, yy):
        @pl.when(zz * ny + yy != me)
        def _():
            for dx in range(1, shares):
                over_x(zz, yy, dx).start()

    f_sems = (None, None, fz_recv, fy_send, fy_recv)
    q_sems = (mu_send.at[0], md_send.at[0], mz_recv.at[0], my_send.at[0], my_recv.at[0])
    o_sems = (mu_send.at[1], md_send.at[1], mz_recv.at[1], my_send.at[1], my_recv.at[1])

    def m_hops(low, high):
        def both(k):
            hops(q_piece, k, k + 1, q_sems)
            hops(o_piece, k, k + 1, o_sems)

        loop(low, high, both)


    def to_z(zz):
        own_piece = f_piece(z, y)
        return remote(own_piece, own_piece, fz_send.at[zz], fz_recv.at[z], zz * ny + y)

    def of_z(zz):
        piece = f_piece(zz, y)
        return remote(piece, piece, fz_send.at[zz], fz_recv.at[zz], zz * ny + y)

    def nearest(act):
        def step(k):
            @pl.when(z >= k)
            def _():
                act(z - k)

            @pl.when(z + k < nz)
            def _():
                act(z + k)

        loop(1, nz, step)

    def pass_f(zz):
        of_z(zz).wait_recv()
        f_onward(zz)

    def f_onward(zz):
        loop(1, ny, lambda dy: along_y(f_piece, zz, dy, f_sems).start())
        send_x(zz, y)

    nearest(lambda zz: to_z(zz).start())
    f_onward(z)
    nearest(pass_f)
    m_hops(0, 1)
    pltpu.make_async_copy(inputs, xbuf, local_sem.at[1]).wait()

    def take_y(zz, dy):
        from_y(f_piece, zz, dy, f_sems).wait_recv()
        send_x(zz, lax.rem(y + ny - dy, ny))

    all_y(take_y)

    def others(act):
        for dx in range(1, shares):
            loop(1, n, lambda i: act(lax.rem(me + i, n) // ny, lax.rem(me + i, ny), dx))

    others(lambda zz, yy, dx: from_x(zz, yy, dx).wait_recv())
    fac = factors.at[core]
    share = remote(fac, fac, fc_sem.at[0], fc_sem.at[1], me, other)
    share.start()

    rank = factors.shape[-1]
    width = inputs.shape[1]
    if factors.shape[3] % 16 == 0:
        table = factors[core].reshape(width, rank)
    else:
        table = factors[core].astype(jnp.float32).reshape(width, rank).astype(jnp.bfloat16)
    tokens = xbuf.shape[0]
    tile = math.gcd(tokens, 256)

    def fold(i, c):
        at = pl.ds(pl.multiple_of(i * tile, tile), tile)
        lows[core, at, :] = jnp.dot(
            xbuf[at, :], table, preferred_element_type=jnp.float32
        ).astype(jnp.bfloat16)
        return c

    lax.fori_loop(0, tokens // tile, fold, 0)
    swap = remote(lows.at[core], lows.at[core], low_sem.at[0], low_sem.at[1], me, other)
    swap.start()
    swap.wait_recv()

    terms[0] = lax.dot_general(lows[0], query_cot[...], contract_rows, preferred_element_type=jnp.float32)
    terms[1] = lax.dot_general(lows[1], head_out[...], contract_rows, preferred_element_type=jnp.float32)
    for j in range(n):
        for w in range(2):
            parts[j, w] = terms[w, j * own:(j + 1) * own, :].astype(jnp.bfloat16)

    def scatter(i):
        f = lax.rem(me + i, n)
        return remote(parts.at[f], got.at[me], rs_send.at[f], rs_recv.at[me], f)

    def scattered(i):
        f = lax.rem(me + i, n)
        return remote(parts.at[f], got.at[f], rs_send.at[f], rs_recv.at[f], f)

    def each(make, act):
        def go(i, c):
            act(make(i))
            return c
        lax.fori_loop(1, n, go, 0)

    each(scatter, lambda d: d.start())
    m_hops(1, 3)
    each(scattered, lambda d: d.wait_recv())
    back = factors.at[1 - core]
    remote(back, back, fc_sem.at[0], fc_sem.at[1], me, other).wait_recv()

    got[me] = parts[me]

    def add(j, c):
        return c + got[j].astype(jnp.float32)

    proj = lax.fori_loop(0, n, add, jnp.zeros(got.shape[1:], jnp.float32))
    sq = proj * proj
    row = jnp.sum(jnp.sum(sq, axis=0), axis=0, keepdims=True)
    squares[mine] = sum(row[:, k:k + 128] for k in range(0, row.shape[1], 128))

    def tell(i, c):
        k = lax.rem(mine + i, total)
        remote(
            squares.at[mine], squares.at[mine], ss_sem.at[0], ss_sem.at[1],
            k // tp, lax.rem(k, tp),
        ).start()
        return c

    lax.fori_loop(1, total, tell, 0)
    rest = squares.at[pl.ds(0, total - 1)]
    pltpu.make_async_copy(rest, rest, ss_sem.at[1]).wait()
    rms = jnp.sqrt(jnp.sum(squares[...]) / count + norm_eps)

    olds = ((query_first, query_second), (out_first, out_second))
    for w in range(2):
        normed = proj[w] / rms
        normed_out[w] = normed
        first, second = moments(normed, olds[w][0][...], olds[w][1][...])
        dirs[me, w] = (first / (jnp.sqrt(second) + adam_eps)).astype(jnp.bfloat16)

    def spread(i):
        f = lax.rem(me + i, n)
        return remote(dirs.at[me], dirs.at[me], ag_send.at[f], ag_recv.at[me], f)

    def arrived(i):
        f = lax.rem(me + i, n)
        return remote(dirs.at[f], dirs.at[f], ag_send.at[f], ag_recv.at[f], f)

    each(spread, lambda d: d.start())
    m_hops(3, nz)
    each(arrived, lambda d: d.wait_recv())
    for w in range(2):
        for j in range(n):
            whole[j * own:(j + 1) * own, :] = dirs[j, w].astype(jnp.float32)
        direction[w] = whole[...].astype(jnp.bfloat16)

    all_y(lambda zz, dy: from_y(q_piece, zz, dy, q_sems).wait_recv())
    all_y(lambda zz, dy: from_y(o_piece, zz, dy, o_sems).wait_recv())
    share.wait_send()
    swap.wait_send()
    nearest(lambda zz: to_z(zz).wait_send())
    all_y(lambda zz, dy: along_y(f_piece, zz, dy, f_sems).wait_send())
    sent(q_piece, q_sems)
    sent(o_piece, o_sems)
    others(lambda zz, yy, dx: over_x(zz, yy, dx).wait_send())
    each(scatter, lambda d: d.wait_send())
    each(spread, lambda d: d.wait_send())
    pltpu.make_async_copy(rest, rest, ss_sem.at[0]).wait()


def exchange(n, tp, inputs, out_cot, query_factor, out_factor, query_cot, head_out,
             query_master, out_master, *olds):
    rows = query_master.shape[0]
    rank = query_factor.shape[-1]
    cols = query_cot.shape[1]
    own = olds[0].shape[0]
    tokens, width = inputs.shape
    nz, ny = split_axis(n)
    vmem = pl.BlockSpec(memory_space=pltpu.VMEM)
    anyspace = pl.BlockSpec(memory_space=pl.ANY)
    dma = pltpu.SemaphoreType.DMA
    bf, f32 = jnp.bfloat16, jnp.float32
    shares = shares_of(tp, rows)
    gather = (dma((nz,)), dma((nz,)), dma((nz, ny)), dma((nz, ny)))
    chunks = (dma((2, nz)), dma((2, nz)), dma((2, nz)), dma((2, nz, ny)), dma((2, nz, ny)))
    shape = jax.ShapeDtypeStruct
    return pl.pallas_call(
        functools.partial(kernel, n, tp, 2.0 * rank * cols * tp),
        out_shape=(
            shape((2, n, shares, rows // shares, rank), bf),
            shape((2, n, rows, cols), bf),
            shape((2, rank, cols), bf),
            shape((2, own, cols), f32),
        ),
        in_specs=[anyspace] * 4 + [vmem] * 8,
        out_specs=(vmem,) * 4,
        scratch_shapes=[
            pltpu.VMEM((tokens, width), bf),
            pltpu.VMEM((2, tokens, rank), bf),
            pltpu.VMEM((2, rank, cols), f32),
            pltpu.VMEM((n, 2, own, cols), bf),
            pltpu.VMEM((n, 2, own, cols), bf),
            pltpu.VMEM((n * tp, 1, 128), f32),
            pltpu.VMEM((n, 2, own, cols), bf),
            pltpu.VMEM((rank, cols), f32),
            dma((2,)), dma((2,)),
            *gather, dma((n, shares)), dma((n, shares)), dma((2,)),
            *chunks,
            dma((n,)), dma((n,)), dma((2,)), dma((n,)), dma((n,)),
        ],
        compiler_params=pltpu.CompilerParams(
            collective_id=0, has_side_effects=True, vmem_limit_bytes=56 * 1024 * 1024
        ),
    )(inputs, out_cot, query_factor, out_factor, query_cot, head_out,
      query_master, out_master, *olds)


def body(
    n, tp, inputs, query_cot, head_out, out_cot, query_factor, out_factor,
    query_master, out_master, query_first, query_second, out_first, out_second,
):
    rows = query_factor.shape[0]
    shares = shares_of(tp, rows)

    def split(factor):
        return factor.reshape(shares, rows // shares, -1)

    factors, masters, direction, normed = exchange(
        n, tp, inputs, out_cot, split(query_factor), split(out_factor), query_cot, head_out,
        query_master, out_master, query_first, query_second, out_first, out_second,
    )
    rank = query_factor.shape[1]
    own, cols = query_first.shape
    f32, bf = jnp.float32, jnp.bfloat16
    factors = factors.reshape(2, n, rows, rank)
    shape = jax.ShapeDtypeStruct

    def fixed(*dims):
        return pl.BlockSpec(dims, lambda j: (0,) * len(dims))

    blocks = n // math.gcd(n, 4)
    block = pl.BlockSpec((blocks * rows, cols), lambda j: (j, 0))
    return pl.pallas_call(
        finish,
        grid=(n // blocks,),
        in_specs=[
            pl.BlockSpec((2, blocks, rows, rank), lambda j: (0, j, 0, 0)),
            pl.BlockSpec((2, blocks, rows, cols), lambda j: (0, j, 0, 0)),
            fixed(2, rank, cols),
            fixed(2, own, cols),
        ] + [fixed(own, cols)] * 4,
        out_specs=[fixed(rows, cols)] * 2 + [block] * 2 + [fixed(own, cols)] * 4,
        out_shape=[shape((rows, cols), f32)] * 2
        + [shape((n * rows, cols), bf)] * 2
        + [shape((own, cols), f32)] * 4,
    )(factors, masters, direction, normed, query_first, query_second, out_first, out_second)


def solution(mesh):
    rows, both = P("fs", None), P("fs", "tp")
    return jax.shard_map(
        functools.partial(body, mesh.shape["fs"], mesh.shape["tp"]),
        mesh=mesh,
        in_specs=(rows, both, both, rows, rows, rows) + (both,) * 6,
        out_specs=(both, both, P(None, "tp"), P(None, "tp")) + (both,) * 4,
        check_vma=False,
    )
```

```python
import functools
import math

import jax
import jax.numpy as jnp
from jax import lax
from jax.experimental import pallas as pl
from jax.experimental.pallas import tpu as pltpu
from jax.sharding import PartitionSpec as P

beta_first = 0.8
beta_second = 0.95
adam_eps = 1e-08
learn_rate = 0.05
norm_eps = 1e-06
contract_rows = (((0,), (0,)), ((), ()))
MESH = pl.DeviceIdType.MESH


def shares_of(tp, rows):
    return tp // 2 if rows % (tp // 2 * 16) == 0 else 1


def split_axis(n):
    ny = max(d for d in range(1, math.isqrt(n) + 1) if n % d == 0)
    return n // ny, ny


def moments(normed, first, second):
    first_new = beta_first * first + (1.0 - beta_first) * normed
    second_new = beta_second * second + (1.0 - beta_second) * normed * normed
    return first_new, second_new


def finish(
    factors, masters, direction, normed, query_first, query_second, out_first, out_second,
    query_step, out_step, query_copy, out_copy, first_q, second_q, first_o, second_o,
):
    j = pl.program_id(0)

    @pl.when(j == 0)
    def _():
        first_q[...], second_q[...] = moments(normed[0], query_first[...], query_second[...])
        first_o[...], second_o[...] = moments(normed[1], out_first[...], out_second[...])

    me = lax.axis_index("fs")
    blocks, rows = factors.shape[1:3]

    def one(i, c):
        at = pl.ds(pl.multiple_of(i * rows, 8), rows)
        for w, (step_out, copy) in enumerate(((query_step, query_copy), (out_step, out_copy))):
            step = jnp.dot(factors[w, i], direction[w], preferred_element_type=jnp.float32)
            copy[at, :] = (masters[w, i].astype(jnp.float32) - learn_rate * step).astype(copy.dtype)

            @pl.when(j * blocks + i == me)
            def _():
                step_out[...] = step
        return c

    if rows % 16 == 0:
        for w, (step_out, copy) in enumerate(((query_step, query_copy), (out_step, out_copy))):
            step = jnp.dot(
                factors[w].reshape(blocks * rows, -1), direction[w], preferred_element_type=jnp.float32
            )
            master = masters[w].reshape(blocks * rows, -1).astype(jnp.float32)
            copy[...] = (master - learn_rate * step).astype(copy.dtype)
            for i in range(blocks):
                @pl.when(j * blocks + i == me)
                def _():
                    step_out[...] = step[i * rows:(i + 1) * rows]
    else:
        lax.fori_loop(0, blocks, one, 0)


def kernel(
    n, tp, count,
    inputs, out_cot, query_factor, out_factor,
    query_cot, head_out, query_master, out_master,
    query_first, query_second, out_first, out_second,
    factors, masters, direction, normed_out,
    xbuf, lows, terms, parts, got, squares, dirs, whole,
    local_sem, low_sem, fz_send, fz_recv, fy_send, fy_recv, fx_send, fx_recv, fc_sem,
    mu_send, md_send, mz_recv, my_send, my_recv, rs_send, rs_recv, ss_sem, ag_send, ag_recv,
):
    nz, ny = split_axis(n)
    me, t = lax.axis_index("fs"), lax.axis_index("tp")
    z, y = me // ny, lax.rem(me, ny)
    core = lax.rem(t, 2)
    other = t + 1 - 2 * core
    total = n * tp
    mine = me * tp + t
    own = query_first.shape[0]

    def own_factor(source):
        return pltpu.make_async_copy(source, factors.at[core, me], local_sem.at[0])

    @pl.when(core == 0)
    def _():
        own_factor(query_factor).start()
        pltpu.make_async_copy(inputs, xbuf, local_sem.at[1]).start()

    @pl.when(core == 1)
    def _():
        own_factor(out_factor).start()
        pltpu.make_async_copy(out_cot, xbuf, local_sem.at[1]).start()

    barrier = pltpu.get_barrier_semaphore()

    def greet(f, tt):
        pl.semaphore_signal(
            barrier, inc=1, device_id={"fs": f, "tp": tt}, device_id_type=MESH
        )

    def loop(low, high, act):
        def go(i, c):
            act(i)
            return c
        lax.fori_loop(low, high, go, 0)

    shares = factors.shape[2]
    if shares == tp // 2:
        loop(1, nz, lambda i: greet(lax.rem(z + i, nz) * ny + y, t))
        loop(1, ny, lambda i: greet(z * ny + lax.rem(y + i, ny), t))
        loop(1, shares, lambda i: greet(me, lax.rem(t + 2 * i, tp)))
        greet(me, other)
        greeted = nz + ny + shares - 2
    else:
        loop(1, total, lambda i: greet(lax.rem(mine + i, total) // tp, lax.rem(mine + i, tp)))
        greeted = total - 1
    masters[0, me] = query_master[...].astype(jnp.bfloat16)
    masters[1, me] = out_master[...].astype(jnp.bfloat16)
    pl.semaphore_wait(barrier, greeted)
    own_factor(query_factor).wait()

    def remote(src, dst, send, recv, f, tt=None):
        where = {"fs": f} if tt is None else {"fs": f, "tp": tt}
        return pltpu.make_async_remote_copy(
            src_ref=src, dst_ref=dst, send_sem=send, recv_sem=recv,
            device_id=where, device_id_type=MESH,
        )

    def up(piece, zz, sems):
        return remote(piece(zz, y), piece(zz, y), sems[0].at[zz], sems[2].at[zz], me + ny)

    def down(piece, zz, sems):
        return remote(piece(zz, y), piece(zz, y), sems[1].at[zz], sems[2].at[zz], me - ny)

    def along_y(piece, zz, dy, sems):
        return remote(
            piece(zz, y), piece(zz, y), sems[3].at[zz, dy], sems[4].at[zz, y],
            z * ny + lax.rem(y + dy, ny),
        )

    def from_y(piece, zz, dy, sems):
        src = lax.rem(y + ny - dy, ny)
        return remote(
            piece(zz, src), piece(zz, src), sems[3].at[zz, dy], sems[4].at[zz, src], z * ny + src
        )

    def hops(piece, low, high, sems):
        def pass_on(zz, come, up_too, down_too):
            @pl.when(come)
            def _():
                @pl.when(zz != z)
                def _():
                    up(piece, zz, sems).wait_recv()

                @pl.when(up_too)
                def _():
                    up(piece, zz, sems).start()

                @pl.when(down_too)
                def _():
                    down(piece, zz, sems).start()

                loop(1, ny, lambda dy: along_y(piece, zz, dy, sems).start())

        def step(k):
            pass_on(z - k, z >= k, z < nz - 1, (k == 0) & (z > 0))
            pass_on(z + k, (k > 0) & (z + k < nz), z < 0, z > 0)

        loop(low, high, step)

    def all_y(act):
        loop(0, nz * (ny - 1), lambda k: act(k // (ny - 1), 1 + lax.rem(k, ny - 1)))

    def sent(piece, sems):
        @pl.when(z < nz - 1)
        def _():
            loop(0, z + 1, lambda zz: up(piece, zz, sems).wait_send())

        @pl.when(z > 0)
        def _():
            loop(z, nz, lambda zz: down(piece, zz, sems).wait_send())

        all_y(lambda zz, dy: along_y(piece, zz, dy, sems).wait_send())

    part = lax.rem(t // 2, shares)

    def f_piece(zz, yy):
        return factors.at[core, zz * ny + yy, part]

    def q_piece(zz, yy):
        return masters.at[0, zz * ny + yy]

    def o_piece(zz, yy):
        return masters.at[1, zz * ny + yy]

    def over_x(zz, yy, dx):
        block = zz * ny + yy
        piece = factors.at[core, block, part]
        return remote(
            piece, piece, fx_send.at[block, dx], fx_recv.at[block, part],
            me, 2 * lax.rem(part + dx, shares) + core,
        )

    def from_x(zz, yy, dx):
        block = zz * ny + yy
        src = lax.rem(part + shares - dx, shares)
        piece = factors.at[core, block, src]
        return remote(
            piece, piece, fx_send.at[block, dx], fx_recv.at[block, src], me, 2 * src + core
        )

    def send_x(zz, yy):
        @pl.when(zz * ny + yy != me)
        def _():
            for dx in range(1, shares):
                over_x(zz, yy, dx).start()

    f_sems = (None, None, fz_recv, fy_send, fy_recv)
    q_sems = (mu_send.at[0], md_send.at[0], mz_recv.at[0], my_send.at[0], my_recv.at[0])
    o_sems = (mu_send.at[1], md_send.at[1], mz_recv.at[1], my_send.at[1], my_recv.at[1])

    def m_hops(low, high):
        def both(k):
            hops(q_piece, k, k + 1, q_sems)
            hops(o_piece, k, k + 1, o_sems)

        loop(low, high, both)


    def to_z(zz):
        own_piece = f_piece(z, y)
        return remote(own_piece, own_piece, fz_send.at[zz], fz_recv.at[z], zz * ny + y)

    def of_z(zz):
        piece = f_piece(zz, y)
        return remote(piece, piece, fz_send.at[zz], fz_recv.at[zz], zz * ny + y)

    def nearest(act):
        def step(k):
            @pl.when(z >= k)
            def _():
                act(z - k)

            @pl.when(z + k < nz)
            def _():
                act(z + k)

        loop(1, nz, step)

    def pass_f(zz):
        of_z(zz).wait_recv()
        f_onward(zz)

    def f_onward(zz):
        loop(1, ny, lambda dy: along_y(f_piece, zz, dy, f_sems).start())
        send_x(zz, y)

    nearest(lambda zz: to_z(zz).start())
    f_onward(z)
    nearest(pass_f)
    m_hops(0, 1)
    pltpu.make_async_copy(inputs, xbuf, local_sem.at[1]).wait()

    def take_y(zz, dy):
        from_y(f_piece, zz, dy, f_sems).wait_recv()
        send_x(zz, lax.rem(y + ny - dy, ny))

    all_y(take_y)

    def others(act):
        for dx in range(1, shares):
            loop(1, n, lambda i: act(lax.rem(me + i, n) // ny, lax.rem(me + i, ny), dx))

    m_hops(1, 2)
    others(lambda zz, yy, dx: from_x(zz, yy, dx).wait_recv())
    fac = factors.at[core]
    share = remote(fac, fac, fc_sem.at[0], fc_sem.at[1], me, other)
    share.start()

    rank = factors.shape[-1]
    width = inputs.shape[1]
    if factors.shape[3] % 16 == 0:
        table = factors[core].reshape(width, rank)
    else:
        table = factors[core].astype(jnp.float32).reshape(width, rank).astype(jnp.bfloat16)
    tokens = xbuf.shape[0]
    tile = math.gcd(tokens, 256)

    def fold(i, c):
        at = pl.ds(pl.multiple_of(i * tile, tile), tile)
        lows[core, at, :] = jnp.dot(
            xbuf[at, :], table, preferred_element_type=jnp.float32
        ).astype(jnp.bfloat16)
        return c

    lax.fori_loop(0, tokens // tile, fold, 0)
    swap = remote(lows.at[core], lows.at[core], low_sem.at[0], low_sem.at[1], me, other)
    swap.start()
    swap.wait_recv()

    terms[0] = lax.dot_general(lows[0], query_cot[...], contract_rows, preferred_element_type=jnp.float32)
    terms[1] = lax.dot_general(lows[1], head_out[...], contract_rows, preferred_element_type=jnp.float32)
    for j in range(n):
        for w in range(2):
            parts[j, w] = terms[w, j * own:(j + 1) * own, :].astype(jnp.bfloat16)

    def scatter(i):
        f = lax.rem(me + i, n)
        return remote(parts.at[f], got.at[me], rs_send.at[f], rs_recv.at[me], f)

    def scattered(i):
        f = lax.rem(me + i, n)
        return remote(parts.at[f], got.at[f], rs_send.at[f], rs_recv.at[f], f)

    def each(make, act):
        def go(i, c):
            act(make(i))
            return c
        lax.fori_loop(1, n, go, 0)

    each(scatter, lambda d: d.start())
    m_hops(2, nz)
    each(scattered, lambda d: d.wait_recv())
    back = factors.at[1 - core]
    remote(back, back, fc_sem.at[0], fc_sem.at[1], me, other).wait_recv()

    got[me] = parts[me]

    def add(j, c):
        return c + got[j].astype(jnp.float32)

    proj = lax.fori_loop(0, n, add, jnp.zeros(got.shape[1:], jnp.float32))
    sq = proj * proj
    row = jnp.sum(jnp.sum(sq, axis=0), axis=0, keepdims=True)
    squares[mine] = sum(row[:, k:k + 128] for k in range(0, row.shape[1], 128))

    def tell(i, c):
        k = lax.rem(mine + i, total)
        remote(
            squares.at[mine], squares.at[mine], ss_sem.at[0], ss_sem.at[1],
            k // tp, lax.rem(k, tp),
        ).start()
        return c

    lax.fori_loop(1, total, tell, 0)
    rest = squares.at[pl.ds(0, total - 1)]
    pltpu.make_async_copy(rest, rest, ss_sem.at[1]).wait()
    rms = jnp.sqrt(jnp.sum(squares[...]) / count + norm_eps)

    olds = ((query_first, query_second), (out_first, out_second))
    for w in range(2):
        normed = proj[w] / rms
        normed_out[w] = normed
        first, second = moments(normed, olds[w][0][...], olds[w][1][...])
        dirs[me, w] = (first / (jnp.sqrt(second) + adam_eps)).astype(jnp.bfloat16)

    def spread(i):
        f = lax.rem(me + i, n)
        return remote(dirs.at[me], dirs.at[me], ag_send.at[f], ag_recv.at[me], f)

    def arrived(i):
        f = lax.rem(me + i, n)
        return remote(dirs.at[f], dirs.at[f], ag_send.at[f], ag_recv.at[f], f)

    each(spread, lambda d: d.start())
    each(arrived, lambda d: d.wait_recv())
    for w in range(2):
        for j in range(n):
            whole[j * own:(j + 1) * own, :] = dirs[j, w].astype(jnp.float32)
        direction[w] = whole[...].astype(jnp.bfloat16)

    all_y(lambda zz, dy: from_y(q_piece, zz, dy, q_sems).wait_recv())
    all_y(lambda zz, dy: from_y(o_piece, zz, dy, o_sems).wait_recv())
    share.wait_send()
    swap.wait_send()
    nearest(lambda zz: to_z(zz).wait_send())
    all_y(lambda zz, dy: along_y(f_piece, zz, dy, f_sems).wait_send())
    sent(q_piece, q_sems)
    sent(o_piece, o_sems)
    others(lambda zz, yy, dx: over_x(zz, yy, dx).wait_send())
    each(scatter, lambda d: d.wait_send())
    each(spread, lambda d: d.wait_send())
    pltpu.make_async_copy(rest, rest, ss_sem.at[0]).wait()


def exchange(n, tp, inputs, out_cot, query_factor, out_factor, query_cot, head_out,
             query_master, out_master, *olds):
    rows = query_master.shape[0]
    rank = query_factor.shape[-1]
    cols = query_cot.shape[1]
    own = olds[0].shape[0]
    tokens, width = inputs.shape
    nz, ny = split_axis(n)
    vmem = pl.BlockSpec(memory_space=pltpu.VMEM)
    anyspace = pl.BlockSpec(memory_space=pl.ANY)
    dma = pltpu.SemaphoreType.DMA
    bf, f32 = jnp.bfloat16, jnp.float32
    shares = shares_of(tp, rows)
    gather = (dma((nz,)), dma((nz,)), dma((nz, ny)), dma((nz, ny)))
    chunks = (dma((2, nz)), dma((2, nz)), dma((2, nz)), dma((2, nz, ny)), dma((2, nz, ny)))
    shape = jax.ShapeDtypeStruct
    return pl.pallas_call(
        functools.partial(kernel, n, tp, 2.0 * rank * cols * tp),
        out_shape=(
            shape((2, n, shares, rows // shares, rank), bf),
            shape((2, n, rows, cols), bf),
            shape((2, rank, cols), bf),
            shape((2, own, cols), f32),
        ),
        in_specs=[anyspace] * 4 + [vmem] * 8,
        out_specs=(vmem,) * 4,
        scratch_shapes=[
            pltpu.VMEM((tokens, width), bf),
            pltpu.VMEM((2, tokens, rank), bf),
            pltpu.VMEM((2, rank, cols), f32),
            pltpu.VMEM((n, 2, own, cols), bf),
            pltpu.VMEM((n, 2, own, cols), bf),
            pltpu.VMEM((n * tp, 1, 128), f32),
            pltpu.VMEM((n, 2, own, cols), bf),
            pltpu.VMEM((rank, cols), f32),
            dma((2,)), dma((2,)),
            *gather, dma((n, shares)), dma((n, shares)), dma((2,)),
            *chunks,
            dma((n,)), dma((n,)), dma((2,)), dma((n,)), dma((n,)),
        ],
        compiler_params=pltpu.CompilerParams(
            collective_id=0, has_side_effects=True, vmem_limit_bytes=56 * 1024 * 1024
        ),
    )(inputs, out_cot, query_factor, out_factor, query_cot, head_out,
      query_master, out_master, *olds)


def body(
    n, tp, inputs, query_cot, head_out, out_cot, query_factor, out_factor,
    query_master, out_master, query_first, query_second, out_first, out_second,
):
    rows = query_factor.shape[0]
    shares = shares_of(tp, rows)

    def split(factor):
        return factor.reshape(shares, rows // shares, -1)

    factors, masters, direction, normed = exchange(
        n, tp, inputs, out_cot, split(query_factor), split(out_factor), query_cot, head_out,
        query_master, out_master, query_first, query_second, out_first, out_second,
    )
    rank = query_factor.shape[1]
    own, cols = query_first.shape
    f32, bf = jnp.float32, jnp.bfloat16
    factors = factors.reshape(2, n, rows, rank)
    shape = jax.ShapeDtypeStruct

    def fixed(*dims):
        return pl.BlockSpec(dims, lambda j: (0,) * len(dims))

    blocks = n // 2
    block = pl.BlockSpec((blocks * rows, cols), lambda j: (j, 0))
    return pl.pallas_call(
        finish,
        grid=(n // blocks,),
        in_specs=[
            pl.BlockSpec((2, blocks, rows, rank), lambda j: (0, j, 0, 0)),
            pl.BlockSpec((2, blocks, rows, cols), lambda j: (0, j, 0, 0)),
            fixed(2, rank, cols),
            fixed(2, own, cols),
        ] + [fixed(own, cols)] * 4,
        out_specs=[fixed(rows, cols)] * 2 + [block] * 2 + [fixed(own, cols)] * 4,
        out_shape=[shape((rows, cols), f32)] * 2
        + [shape((n * rows, cols), bf)] * 2
        + [shape((own, cols), f32)] * 4,
    )(factors, masters, direction, normed, query_first, query_second, out_first, out_second)


def solution(mesh):
    rows, both = P("fs", None), P("fs", "tp")
    return jax.shard_map(
        functools.partial(body, mesh.shape["fs"], mesh.shape["tp"]),
        mesh=mesh,
        in_specs=(rows, both, both, rows, rows, rows) + (both,) * 6,
        out_specs=(both, both, P(None, "tp"), P(None, "tp")) + (both,) * 4,
        check_vma=False,
    )
```

```python
import functools
import math

import jax
import jax.numpy as jnp
from jax import lax
from jax.experimental import pallas as pl
from jax.experimental.pallas import tpu as pltpu
from jax.sharding import PartitionSpec as P

beta_first = 0.8
beta_second = 0.95
adam_eps = 1e-08
learn_rate = 0.05
norm_eps = 1e-06
contract_rows = (((0,), (0,)), ((), ()))
MESH = pl.DeviceIdType.MESH


def shares_of(tp, rows):
    return tp // 2 if rows % (tp // 2 * 16) == 0 else 1


def split_axis(n):
    ny = max(d for d in range(1, math.isqrt(n) + 1) if n % d == 0)
    return n // ny, ny


def moments(normed, first, second):
    first_new = beta_first * first + (1.0 - beta_first) * normed
    second_new = beta_second * second + (1.0 - beta_second) * normed * normed
    return first_new, second_new


def finish(
    factors, masters, direction, normed, query_first, query_second, out_first, out_second,
    query_step, out_step, query_copy, out_copy, first_q, second_q, first_o, second_o,
):
    j = pl.program_id(0)

    @pl.when(j == 0)
    def _():
        first_q[...], second_q[...] = moments(normed[0], query_first[...], query_second[...])
        first_o[...], second_o[...] = moments(normed[1], out_first[...], out_second[...])

    me = lax.axis_index("fs")
    blocks, rows = factors.shape[1:3]

    def one(i, c):
        at = pl.ds(pl.multiple_of(i * rows, 8), rows)
        for w, (step_out, copy) in enumerate(((query_step, query_copy), (out_step, out_copy))):
            step = jnp.dot(factors[w, i], direction[w], preferred_element_type=jnp.float32)
            copy[at, :] = (masters[w, i].astype(jnp.float32) - learn_rate * step).astype(copy.dtype)

            @pl.when(j * blocks + i == me)
            def _():
                step_out[...] = step
        return c

    if rows % 16 == 0:
        for w, (step_out, copy) in enumerate(((query_step, query_copy), (out_step, out_copy))):
            step = jnp.dot(
                factors[w].reshape(blocks * rows, -1), direction[w], preferred_element_type=jnp.float32
            )
            master = masters[w].reshape(blocks * rows, -1).astype(jnp.float32)
            copy[...] = (master - learn_rate * step).astype(copy.dtype)
            for i in range(blocks):
                @pl.when(j * blocks + i == me)
                def _():
                    step_out[...] = step[i * rows:(i + 1) * rows]
    else:
        lax.fori_loop(0, blocks, one, 0)


def kernel(
    n, tp, count,
    inputs, out_cot, query_factor, out_factor,
    query_cot, head_out, query_master, out_master,
    query_first, query_second, out_first, out_second,
    factors_out, masters_out, direction, normed_out,
    factors, masters, cots, fulls, olds, xbuf, lows, terms, parts, got, squares, dirs, whole,
    local_sem, in_sem, out_sem, low_sem, fz_send, fz_recv, fy_send, fy_recv, fx_send, fx_recv, fc_sem,
    mu_send, md_send, mz_recv, my_send, my_recv, rs_send, rs_recv, ss_sem, ag_send, ag_recv,
):
    nz, ny = split_axis(n)
    me, t = lax.axis_index("fs"), lax.axis_index("tp")
    z, y = me // ny, lax.rem(me, ny)
    core = lax.rem(t, 2)
    other = t + 1 - 2 * core
    total = n * tp
    mine = me * tp + t
    own = query_first.shape[0]

    def own_factor(source):
        return pltpu.make_async_copy(source, factors.at[core, me], local_sem.at[0])

    @pl.when(core == 0)
    def _():
        own_factor(query_factor).start()
        pltpu.make_async_copy(inputs, xbuf, local_sem.at[1]).start()

    @pl.when(core == 1)
    def _():
        own_factor(out_factor).start()
        pltpu.make_async_copy(out_cot, xbuf, local_sem.at[1]).start()

    barrier = pltpu.get_barrier_semaphore()

    def greet(f, tt):
        pl.semaphore_signal(
            barrier, inc=1, device_id={"fs": f, "tp": tt}, device_id_type=MESH
        )

    def loop(low, high, act):
        def go(i, c):
            act(i)
            return c
        lax.fori_loop(low, high, go, 0)

    shares = factors.shape[2]
    if shares == tp // 2:
        loop(1, nz, lambda i: greet(lax.rem(z + i, nz) * ny + y, t))
        loop(1, ny, lambda i: greet(z * ny + lax.rem(y + i, ny), t))
        loop(1, shares, lambda i: greet(me, lax.rem(t + 2 * i, tp)))
        greet(me, other)
        greeted = nz + ny + shares - 2
    else:
        loop(1, total, lambda i: greet(lax.rem(mine + i, total) // tp, lax.rem(mine + i, tp)))
        greeted = total - 1
    loads = [
        pltpu.make_async_copy(source, target, in_sem.at[k])
        for k, (source, target) in enumerate((
            (query_master, fulls.at[0]), (out_master, fulls.at[1]),
            (query_cot, cots.at[0]), (head_out, cots.at[1]),
            (query_first, olds.at[0]), (query_second, olds.at[1]),
            (out_first, olds.at[2]), (out_second, olds.at[3]),
        ))
    ]
    for load in loads:
        load.start()
    for w in range(2):
        loads[w].wait()
        masters[w, me] = fulls[w].astype(jnp.bfloat16)
    pl.semaphore_wait(barrier, greeted)
    own_factor(query_factor).wait()

    def remote(src, dst, send, recv, f, tt=None):
        where = {"fs": f} if tt is None else {"fs": f, "tp": tt}
        return pltpu.make_async_remote_copy(
            src_ref=src, dst_ref=dst, send_sem=send, recv_sem=recv,
            device_id=where, device_id_type=MESH,
        )

    def up(piece, zz, sems):
        return remote(piece(zz, y), piece(zz, y), sems[0].at[zz], sems[2].at[zz], me + ny)

    def down(piece, zz, sems):
        return remote(piece(zz, y), piece(zz, y), sems[1].at[zz], sems[2].at[zz], me - ny)

    def along_y(piece, zz, dy, sems):
        return remote(
            piece(zz, y), piece(zz, y), sems[3].at[zz, dy], sems[4].at[zz, y],
            z * ny + lax.rem(y + dy, ny),
        )

    def from_y(piece, zz, dy, sems):
        src = lax.rem(y + ny - dy, ny)
        return remote(
            piece(zz, src), piece(zz, src), sems[3].at[zz, dy], sems[4].at[zz, src], z * ny + src
        )

    def hops(piece, low, high, sems):
        def pass_on(zz, come, up_too, down_too):
            @pl.when(come)
            def _():
                @pl.when(zz != z)
                def _():
                    up(piece, zz, sems).wait_recv()

                @pl.when(up_too)
                def _():
                    up(piece, zz, sems).start()

                @pl.when(down_too)
                def _():
                    down(piece, zz, sems).start()

                loop(1, ny, lambda dy: along_y(piece, zz, dy, sems).start())

        def step(k):
            pass_on(z - k, z >= k, z < nz - 1, (k == 0) & (z > 0))
            pass_on(z + k, (k > 0) & (z + k < nz), z < 0, z > 0)

        loop(low, high, step)

    def all_y(act):
        loop(0, nz * (ny - 1), lambda k: act(k // (ny - 1), 1 + lax.rem(k, ny - 1)))

    def sent(piece, sems):
        @pl.when(z < nz - 1)
        def _():
            loop(0, z + 1, lambda zz: up(piece, zz, sems).wait_send())

        @pl.when(z > 0)
        def _():
            loop(z, nz, lambda zz: down(piece, zz, sems).wait_send())

        all_y(lambda zz, dy: along_y(piece, zz, dy, sems).wait_send())

    part = lax.rem(t // 2, shares)

    def f_piece(zz, yy):
        return factors.at[core, zz * ny + yy, part]

    def q_piece(zz, yy):
        return masters.at[0, zz * ny + yy]

    def o_piece(zz, yy):
        return masters.at[1, zz * ny + yy]

    def over_x(zz, yy, dx):
        block = zz * ny + yy
        piece = factors.at[core, block, part]
        return remote(
            piece, piece, fx_send.at[block, dx], fx_recv.at[block, part],
            me, 2 * lax.rem(part + dx, shares) + core,
        )

    def from_x(zz, yy, dx):
        block = zz * ny + yy
        src = lax.rem(part + shares - dx, shares)
        piece = factors.at[core, block, src]
        return remote(
            piece, piece, fx_send.at[block, dx], fx_recv.at[block, src], me, 2 * src + core
        )

    def send_x(zz, yy):
        @pl.when(zz * ny + yy != me)
        def _():
            for dx in range(1, shares):
                over_x(zz, yy, dx).start()

    f_sems = (None, None, fz_recv, fy_send, fy_recv)
    q_sems = (mu_send.at[0], md_send.at[0], mz_recv.at[0], my_send.at[0], my_recv.at[0])
    o_sems = (mu_send.at[1], md_send.at[1], mz_recv.at[1], my_send.at[1], my_recv.at[1])

    def m_hops(low, high):
        def both(k):
            hops(q_piece, k, k + 1, q_sems)
            hops(o_piece, k, k + 1, o_sems)

        loop(low, high, both)


    def to_z(zz):
        own_piece = f_piece(z, y)
        return remote(own_piece, own_piece, fz_send.at[zz], fz_recv.at[z], zz * ny + y)

    def of_z(zz):
        piece = f_piece(zz, y)
        return remote(piece, piece, fz_send.at[zz], fz_recv.at[zz], zz * ny + y)

    def nearest(act):
        def step(k):
            @pl.when(z >= k)
            def _():
                act(z - k)

            @pl.when(z + k < nz)
            def _():
                act(z + k)

        loop(1, nz, step)

    def pass_f(zz):
        of_z(zz).wait_recv()
        f_onward(zz)

    def f_onward(zz):
        loop(1, ny, lambda dy: along_y(f_piece, zz, dy, f_sems).start())
        send_x(zz, y)

    nearest(lambda zz: to_z(zz).start())
    f_onward(z)
    nearest(pass_f)
    m_hops(0, 1)
    pltpu.make_async_copy(inputs, xbuf, local_sem.at[1]).wait()

    def take_y(zz, dy):
        from_y(f_piece, zz, dy, f_sems).wait_recv()
        send_x(zz, lax.rem(y + ny - dy, ny))

    all_y(take_y)

    def others(act):
        for dx in range(1, shares):
            loop(1, n, lambda i: act(lax.rem(me + i, n) // ny, lax.rem(me + i, ny), dx))

    m_hops(1, 2)
    others(lambda zz, yy, dx: from_x(zz, yy, dx).wait_recv())
    fac = factors.at[core]
    share = remote(fac, fac, fc_sem.at[0], fc_sem.at[1], me, other)
    share.start()

    rank = factors.shape[-1]
    width = inputs.shape[1]
    if factors.shape[3] % 16 == 0:
        table = factors[core].reshape(width, rank)
    else:
        table = factors[core].astype(jnp.float32).reshape(width, rank).astype(jnp.bfloat16)
    tokens = xbuf.shape[0]
    tile = math.gcd(tokens, 512)

    def fold(i, c):
        at = pl.ds(pl.multiple_of(i * tile, tile), tile)
        lows[core, at, :] = jnp.dot(
            xbuf[at, :], table, preferred_element_type=jnp.float32
        ).astype(jnp.bfloat16)
        return c

    lax.fori_loop(0, tokens // tile, fold, 0)
    swap = remote(lows.at[core], lows.at[core], low_sem.at[0], low_sem.at[1], me, other)
    swap.start()
    swap.wait_recv()

    for load in loads[2:]:
        load.wait()
    terms[0] = lax.dot_general(lows[0], cots[0], contract_rows, preferred_element_type=jnp.float32)
    terms[1] = lax.dot_general(lows[1], cots[1], contract_rows, preferred_element_type=jnp.float32)
    for j in range(n):
        for w in range(2):
            parts[j, w] = terms[w, j * own:(j + 1) * own, :].astype(jnp.bfloat16)

    def scatter(i):
        f = lax.rem(me + i, n)
        return remote(parts.at[f], got.at[me], rs_send.at[f], rs_recv.at[me], f)

    def scattered(i):
        f = lax.rem(me + i, n)
        return remote(parts.at[f], got.at[f], rs_send.at[f], rs_recv.at[f], f)

    def each(make, act):
        def go(i, c):
            act(make(i))
            return c
        lax.fori_loop(1, n, go, 0)

    each(scatter, lambda d: d.start())
    m_hops(2, 3)
    each(scattered, lambda d: d.wait_recv())
    back = factors.at[1 - core]
    remote(back, back, fc_sem.at[0], fc_sem.at[1], me, other).wait_recv()
    put_factors = pltpu.make_async_copy(factors, factors_out, out_sem.at[0])
    put_factors.start()

    got[me] = parts[me]

    def add(j, c):
        return c + got[j].astype(jnp.float32)

    proj = lax.fori_loop(0, n, add, jnp.zeros(got.shape[1:], jnp.float32))
    sq = proj * proj
    row = jnp.sum(jnp.sum(sq, axis=0), axis=0, keepdims=True)
    squares[mine] = sum(row[:, k:k + 128] for k in range(0, row.shape[1], 128))

    def tell(i, c):
        k = lax.rem(mine + i, total)
        remote(
            squares.at[mine], squares.at[mine], ss_sem.at[0], ss_sem.at[1],
            k // tp, lax.rem(k, tp),
        ).start()
        return c

    lax.fori_loop(1, total, tell, 0)
    m_hops(3, nz)
    rest = squares.at[pl.ds(0, total - 1)]
    pltpu.make_async_copy(rest, rest, ss_sem.at[1]).wait()
    rms = jnp.sqrt(jnp.sum(squares[...]) / count + norm_eps)

    for w in range(2):
        normed = proj[w] / rms
        normed_out[w] = normed
        first, second = moments(normed, olds[2 * w], olds[2 * w + 1])
        dirs[me, w] = (first / (jnp.sqrt(second) + adam_eps)).astype(jnp.bfloat16)

    def spread(i):
        f = lax.rem(me + i, n)
        return remote(dirs.at[me], dirs.at[me], ag_send.at[f], ag_recv.at[me], f)

    def arrived(i):
        f = lax.rem(me + i, n)
        return remote(dirs.at[f], dirs.at[f], ag_send.at[f], ag_recv.at[f], f)

    each(spread, lambda d: d.start())
    each(arrived, lambda d: d.wait_recv())
    for w in range(2):
        for j in range(n):
            whole[j * own:(j + 1) * own, :] = dirs[j, w].astype(jnp.float32)
        direction[w] = whole[...].astype(jnp.bfloat16)

    all_y(lambda zz, dy: from_y(q_piece, zz, dy, q_sems).wait_recv())
    put_q = pltpu.make_async_copy(masters.at[0], masters_out.at[0], out_sem.at[1])
    put_q.start()
    all_y(lambda zz, dy: from_y(o_piece, zz, dy, o_sems).wait_recv())
    put_o = pltpu.make_async_copy(masters.at[1], masters_out.at[1], out_sem.at[2])
    put_o.start()
    share.wait_send()
    swap.wait_send()
    nearest(lambda zz: to_z(zz).wait_send())
    all_y(lambda zz, dy: along_y(f_piece, zz, dy, f_sems).wait_send())
    sent(q_piece, q_sems)
    sent(o_piece, o_sems)
    others(lambda zz, yy, dx: over_x(zz, yy, dx).wait_send())
    each(scatter, lambda d: d.wait_send())
    each(spread, lambda d: d.wait_send())
    pltpu.make_async_copy(rest, rest, ss_sem.at[0]).wait()
    put_factors.wait()
    put_q.wait()
    put_o.wait()


def exchange(n, tp, inputs, out_cot, query_factor, out_factor, query_cot, head_out,
             query_master, out_master, *olds):
    rows = query_master.shape[0]
    rank = query_factor.shape[-1]
    cols = query_cot.shape[1]
    own = olds[0].shape[0]
    tokens, width = inputs.shape
    nz, ny = split_axis(n)
    vmem = pl.BlockSpec(memory_space=pltpu.VMEM)
    anyspace = pl.BlockSpec(memory_space=pl.ANY)
    dma = pltpu.SemaphoreType.DMA
    bf, f32 = jnp.bfloat16, jnp.float32
    shares = shares_of(tp, rows)
    gather = (dma((nz,)), dma((nz,)), dma((nz, ny)), dma((nz, ny)))
    chunks = (dma((2, nz)), dma((2, nz)), dma((2, nz)), dma((2, nz, ny)), dma((2, nz, ny)))
    shape = jax.ShapeDtypeStruct
    return pl.pallas_call(
        functools.partial(kernel, n, tp, 2.0 * rank * cols * tp),
        out_shape=(
            shape((2, n, shares, rows // shares, rank), bf),
            shape((2, n, rows, cols), bf),
            shape((2, rank, cols), bf),
            shape((2, own, cols), f32),
        ),
        in_specs=[anyspace] * 12,
        out_specs=(anyspace, anyspace, vmem, vmem),
        scratch_shapes=[
            pltpu.VMEM((2, n, shares, rows // shares, rank), bf),
            pltpu.VMEM((2, n, rows, cols), bf),
            pltpu.VMEM((2, tokens, cols), bf),
            pltpu.VMEM((2, rows, cols), f32),
            pltpu.VMEM((4, own, cols), f32),
            pltpu.VMEM((tokens, width), bf),
            pltpu.VMEM((2, tokens, rank), bf),
            pltpu.VMEM((2, rank, cols), f32),
            pltpu.VMEM((n, 2, own, cols), bf),
            pltpu.VMEM((n, 2, own, cols), bf),
            pltpu.VMEM((n * tp, 1, 128), f32),
            pltpu.VMEM((n, 2, own, cols), bf),
            pltpu.VMEM((rank, cols), f32),
            dma((2,)), dma((8,)), dma((3,)), dma((2,)),
            *gather, dma((n, shares)), dma((n, shares)), dma((2,)),
            *chunks,
            dma((n,)), dma((n,)), dma((2,)), dma((n,)), dma((n,)),
        ],
        compiler_params=pltpu.CompilerParams(
            collective_id=0, has_side_effects=True, vmem_limit_bytes=56 * 1024 * 1024
        ),
    )(inputs, out_cot, query_factor, out_factor, query_cot, head_out,
      query_master, out_master, *olds)


def body(
    n, tp, inputs, query_cot, head_out, out_cot, query_factor, out_factor,
    query_master, out_master, query_first, query_second, out_first, out_second,
):
    rows = query_factor.shape[0]
    shares = shares_of(tp, rows)

    def split(factor):
        return factor.reshape(shares, rows // shares, -1)

    factors, masters, direction, normed = exchange(
        n, tp, inputs, out_cot, split(query_factor), split(out_factor), query_cot, head_out,
        query_master, out_master, query_first, query_second, out_first, out_second,
    )
    rank = query_factor.shape[1]
    own, cols = query_first.shape
    f32, bf = jnp.float32, jnp.bfloat16
    factors = factors.reshape(2, n, rows, rank)
    shape = jax.ShapeDtypeStruct

    def fixed(*dims):
        return pl.BlockSpec(dims, lambda j: (0,) * len(dims))

    blocks = n // 2
    block = pl.BlockSpec((blocks * rows, cols), lambda j: (j, 0))
    return pl.pallas_call(
        finish,
        grid=(n // blocks,),
        in_specs=[
            pl.BlockSpec((2, blocks, rows, rank), lambda j: (0, j, 0, 0)),
            pl.BlockSpec((2, blocks, rows, cols), lambda j: (0, j, 0, 0)),
            fixed(2, rank, cols),
            fixed(2, own, cols),
        ] + [fixed(own, cols)] * 4,
        out_specs=[fixed(rows, cols)] * 2 + [block] * 2 + [fixed(own, cols)] * 4,
        out_shape=[shape((rows, cols), f32)] * 2
        + [shape((n * rows, cols), bf)] * 2
        + [shape((own, cols), f32)] * 4,
    )(factors, masters, direction, normed, query_first, query_second, out_first, out_second)


def solution(mesh):
    rows, both = P("fs", None), P("fs", "tp")
    return jax.shard_map(
        functools.partial(body, mesh.shape["fs"], mesh.shape["tp"]),
        mesh=mesh,
        in_specs=(rows, both, both, rows, rows, rows) + (both,) * 6,
        out_specs=(both, both, P(None, "tp"), P(None, "tp")) + (both,) * 4,
        check_vma=False,
    )
```
